32 devices in a mesh: grp: 2 (over y), sp: 4 (over z), tp: 4 (over x, core).
Axes of the slice: x: 2, y: 2, z: 4, core: 2. Of those that a mesh axis runs over, the one named last changes fastest.
Arguments:
- tokens: bfloat16 [2, 2048, 2048], P('grp', ('sp', 'tp')), parts along dimension 0, may hold values from -6 to 6
- norm_gain: bfloat16 [2048], replicated, may hold values from 0.099609375 to 1.8984375
- w_query: bfloat16 [2048, 1024], P('sp'), may hold values from -0.125 to 0.125
- w_forget: bfloat16 [2048, 1024], P('sp'), may hold values from -0.125 to 0.125
- w_input: bfloat16 [2048, 1024], P('sp'), may hold values from -0.125 to 0.125
- floor_gap: float32 [1024], replicated, may hold values from 0.000146484375 to 0.12
- extra_decay: float32 [2, 2048, 16], P('grp', ('sp', 'tp')), parts along dimension 0, may hold values from -1.4 to 0, as said below
- init_state: float32 [2, 16, 64, 64], P('grp'), parts along dimension 0, may hold values from -0.078125 to 0.078125
- head_norm_gain: bfloat16 [1024], replicated, may hold values from 0.099609375 to 1.8984375
- w_output: bfloat16 [1024, 2048], P(None, 'sp'), may hold values from -0.1875 to 0.1875
Outputs:
- mixed: bfloat16 [2, 2048, 2048], P('grp', ('sp', 'tp')), parts along dimension 0
- final_state: float32 [2, 65536], P('grp', ('sp', 'tp')), parts along dimension 0
The draws below stay inside these ranges and needn't reach their ends.
There are 2 independent parts, one for each index of `grp`. The reference program is written for one: setup_inputs(seed, part) draws one part's arguments, and reference() takes and returns one part's arrays. A program takes and returns all parts, laid end to end along the dimension named above; an argument that names none is the same for every part. Nothing has to cross between parts.
Inputs may be any that keep to these rules, and one draw needn't show every extreme that they name: `extra_decay`: no entry is positive.
All inputs are finite; a program needn't handle non-finite values.
Results may differ from the reference program's by a relative error of at most 0.014.
Values may be sent and summed in bfloat16 or wider, within the bound.
A program may use at most 128 MiB of HBM per device.

```python
import math
import jax
import jax.numpy as jnp
from jax import lax

D = 2048
HEADS = 16
HEAD = 64
WIDTH = 1024
BLOCK = 64
SEQS = 1
SPAN = 128
POSITION_COUNT = 2048


def draw_floor_gap(key, part):
    order = jax.random.permutation(jax.random.fold_in(key, 11), HEADS)
    rapid = order < HEADS // 2
    rapid_gap = jnp.exp(jax.random.uniform(jax.random.fold_in(key, 12), (HEADS, HEAD), jnp.float32, math.log(0.04), math.log(0.12)))
    steady_gap = jnp.exp(jax.random.uniform(jax.random.fold_in(key, 13), (HEADS, HEAD), jnp.float32, math.log(0.3), 0.0)) / POSITION_COUNT
    return jnp.where(rapid[:, None], rapid_gap, steady_gap).reshape(HEADS * HEAD).astype(jnp.float32)


def draw_extra_decay(key, part):
    pieces = POSITION_COUNT // SPAN
    factor = jnp.exp(jax.random.uniform(jax.random.fold_in(key, 21), (SEQS, pieces, 1, HEADS), jnp.float32, 0.0, math.log(4.0)))
    stable_occasions = -(0.3 / POSITION_COUNT) * jnp.broadcast_to(factor, (SEQS, pieces, SPAN, HEADS)).reshape(SEQS, POSITION_COUNT, HEADS)
    spots = jax.random.randint(jax.random.fold_in(key, 22), (SEQS, 1, HEADS, 2), 0, POSITION_COUNT)
    loss_occasions = jnp.log(jax.random.uniform(jax.random.fold_in(key, 23), (SEQS, 1, HEADS, 2), jnp.float32, 0.5, 0.8))
    strike_occasions = jnp.arange(POSITION_COUNT)[None, :, None, None] == spots
    rapid_occasions = jnp.sum(jnp.where(strike_occasions, loss_occasions, 0.0), axis=3)
    return (stable_occasions + rapid_occasions).astype(jnp.float32)


def block_scale(own_key, extent, shards, smallest, largest):
    level, own = 1.0, jax.random.fold_in(own_key, 6)
    for dim, parts in shards:
        draws = jnp.exp(jax.random.uniform(jax.random.fold_in(own, dim), (parts,), jnp.float32, smallest / len(shards), largest / len(shards)))
        level = level * jnp.repeat(draws, extent[dim] // parts).reshape([-1 if axis == dim else 1 for axis in range(len(extent))])
    return level


def centred(rng, shape, scale, reach, cuts=(), held_as=jnp.bfloat16):
    level = block_scale(rng, shape, cuts, -0.22, 0.18) if cuts else 1.0
    values = jax.random.normal(rng, shape, jnp.float32) * scale * level
    return jnp.minimum(jnp.maximum(values, -reach), reach).astype(held_as)


def setup_inputs(seed: int = 0, part: int = 0) -> dict:
    splits = jax.random.split(jax.random.key(seed), 11)
    own_keys = jax.random.split(jax.random.fold_in(splits[10], part), 11)
    return {
        "tokens": centred(own_keys[0], (SEQS, POSITION_COUNT, D), 1.0, 6.0, ((1, 16),)),
        "norm_gain": jnp.clip(1.0 + 0.18 * jax.random.normal(splits[1], (D,), jnp.float32), 0.099609375, 1.8984375).astype(jnp.bfloat16),
        "w_query": centred(splits[2], (D, WIDTH), D ** -0.5, 0.125, ((0, 4),)),
        "w_forget": centred(splits[3], (D, WIDTH), D ** -0.5, 0.125, ((0, 4),)),
        "w_input": centred(splits[4], (D, WIDTH), D ** -0.5, 0.125, ((0, 4),)),
        "floor_gap": draw_floor_gap(jax.random.fold_in(splits[10], 71), part),
        "extra_decay": draw_extra_decay(jax.random.fold_in(jax.random.fold_in(splits[10], part), 71), part),
        "init_state": centred(own_keys[7], (SEQS, HEADS, HEAD, HEAD), (0.25 / POSITION_COUNT ** 0.5), 0.078125, (), jnp.float32),
        "head_norm_gain": jnp.clip(1.0 + 0.18 * jax.random.normal(splits[8], (WIDTH,), jnp.float32), 0.099609375, 1.8984375).astype(jnp.bfloat16),
        "w_output": centred(splits[9], (WIDTH, D), WIDTH ** -0.5, 0.1875, ((1, 4),)),
    }


EPSILON = 1e-05

def layer_normed(tokens, norm_gain):
    values = tokens.astype(jnp.float32)
    center = values - lax.optimization_barrier(jnp.mean(values, axis=-1, keepdims=True))
    spread = lax.optimization_barrier(jnp.mean(center * center, axis=-1, keepdims=True))
    return (center * lax.rsqrt(spread + EPSILON) * norm_gain.astype(jnp.float32)).astype(jnp.bfloat16)

def gate_terms(normed, w_query, w_forget, w_input, floor_gap, extra_decay):
    query_raw = jnp.dot(normed, w_query, preferred_element_type=jnp.float32).astype(jnp.bfloat16)
    forget_raw = jnp.dot(normed, w_forget, preferred_element_type=jnp.float32).astype(jnp.bfloat16)
    input_raw = jnp.dot(normed, w_input, preferred_element_type=jnp.float32).astype(jnp.bfloat16)
    forget_pre = forget_raw.astype(jnp.float32)
    split_shape = forget_pre.shape[:-1] + (HEADS, HEAD)
    log_keep = jnp.logaddexp(jnp.log1p(-floor_gap), jnp.log(floor_gap) + jax.nn.log_sigmoid(forget_pre))
    log_keep = log_keep.reshape(split_shape) + extra_decay[..., None]
    key_gate = (floor_gap * jax.nn.sigmoid(-forget_pre)).reshape(split_shape)
    query = jax.nn.silu(query_raw.astype(jnp.float32)).reshape(split_shape)
    values = input_raw.astype(jnp.float32).reshape(split_shape)
    return (query, key_gate, values, log_keep)

def reference(tokens, norm_gain, w_query, w_forget, w_input, floor_gap, extra_decay, init_state, head_norm_gain, w_output):
    normed = layer_normed(tokens, norm_gain)
    query, key_gate, values, log_keep = gate_terms(normed, w_query, w_forget, w_input, floor_gap, extra_decay)
    seqs, length_total = (tokens.shape[0], tokens.shape[1])
    blocks = length_total // BLOCK
    causal = lax.broadcasted_iota(jnp.int32, (BLOCK, BLOCK), 0) >= lax.broadcasted_iota(jnp.int32, (BLOCK, BLOCK), 1)
    highest = lax.Precision.HIGHEST

    def to_blocks(array):
        return jnp.moveaxis(array.reshape(seqs, blocks, BLOCK, HEADS, HEAD), 1, 0)

    def advance(state, inputs):
        q_block, k_block, v_block, l_block = inputs
        cumul = jnp.cumsum(l_block, axis=1)
        q_decayed = q_block * jnp.exp(cumul)
        key_decayed = k_block * jnp.exp(-cumul)
        scores = jnp.einsum('sthd,suhd->shtu', q_decayed, key_decayed, precision=highest)
        scores = jnp.where(causal, scores, 0.0)
        within = jnp.einsum('shtu,suhe->sthe', scores, v_block, precision=highest)
        across = jnp.einsum('sthd,shde->sthe', q_decayed, state, precision=highest)
        totals = cumul[:, -1]
        k_tail = k_block * jnp.exp(totals[:, None] - cumul)
        updated_state = jnp.exp(totals)[..., None] * state + jnp.einsum('sthd,sthe->shde', k_tail, v_block, precision=highest)
        return (updated_state, within + across)
    final_state, outputs = lax.scan(advance, init_state, (to_blocks(query), to_blocks(key_gate), to_blocks(values), to_blocks(log_keep)))
    recurrent = jnp.moveaxis(outputs, 0, 1).reshape(seqs, length_total, HEADS, HEAD)
    average_power = lax.optimization_barrier(jnp.mean(recurrent * recurrent, axis=-1, keepdims=True))
    scaled = recurrent * lax.rsqrt(average_power + EPSILON) * head_norm_gain.astype(jnp.float32).reshape(HEADS, HEAD)
    gated = scaled.reshape(seqs, length_total, HEADS * HEAD).astype(jnp.bfloat16)
    mixed = jnp.dot(gated, w_output, preferred_element_type=jnp.float32).astype(jnp.bfloat16)
    return (mixed, final_state.reshape(seqs, HEADS * HEAD * HEAD))
```

```python
import functools

import jax
import jax.numpy as jnp
from jax import lax
from jax.experimental import pallas as pl
from jax.experimental.pallas import tpu as pltpu
from jax.sharding import PartitionSpec as P

HEAD = 64
BLOCK = 64
CORES = 2
LANES = 128
EPSILON = 1e-05
F32, BF16 = jnp.float32, jnp.bfloat16
HIGHEST = lax.Precision.HIGHEST


def contract(a, b, da, db, precision=None):
    return lax.dot_general(
        a, b, (((da,), (db,)), ((), ())), precision=precision, preferred_element_type=F32
    )


def iota(shape, dim):
    return lax.broadcasted_iota(jnp.int32, shape, dim)


def same_group(rows, cols, size):
    return iota((rows, cols), 0) // size == iota((rows, cols), 1) // size


def swap_halves(a):
    return jnp.concatenate([a[:, HEAD:], a[:, :HEAD]], axis=1)


def kernel(
    sizes,
    tokens, norm_gain, w_query, w_forget, w_input, gap, extra, init, head_gain, w_output,
    mixed, final,
    tok, ext, nrm, wbuf, wout, start, qd, kd, val, etot, bstate, within, gated, carried,
    st_send, st_recv, dk_send, dk_recv, fin, fin_recv, a_send, a_recv, b_send, b_recv,
    loc, tok_s, tok_r, ext_s, ext_r, z_s, z_r, y_s, y_r, oz_s, oz_r, oy_s, oy_r,
    st_s, st_r, dk_s, dk_r, fin_s, fin_r, as_, ar_, bs_, br_,
):
    ng, ns, nt, span, D, C, O, chunks = sizes
    g, s, t = lax.axis_index("grp"), lax.axis_index("sp"), lax.axis_index("tp")
    R, OC = D // ns, O // ns
    Rh, Ch = R // ng, C // ng
    nx = nt // CORES
    T = nt * span
    nblk, per = T // BLOCK, span // BLOCK
    G = C // LANES
    fold = G % 2 == 0
    weights = (w_query, w_forget, w_input)
    own_cols = pl.ds(pl.multiple_of(t * C, LANES), C)

    def remote(src, dst, ssem, rsem, where):
        return pltpu.make_async_remote_copy(
            src_ref=src, dst_ref=dst, send_sem=ssem, recv_sem=rsem,
            device_id=where, device_id_type=pl.DeviceIdType.MESH,
        )

    def piece(k, a, who):
        return wbuf.at[pl.ds(pl.multiple_of(k * R + who * Rh, 16), Rh), pl.ds(a * C, C)]

    def z_copy(k, a, way, src):
        to = s + 1 if way == 0 else s - 1
        return remote(src, piece(k, a, g), z_s.at[way, k, a], z_r.at[k, a], {"sp": to})

    def y_copy(k, a, dy, who):
        return remote(
            piece(k, a, who), piece(k, a, who), y_s.at[dy - 1, k, a], y_r.at[dy - 1, k, a],
            {"grp": lax.rem(g + dy, ng)},
        )

    def o_piece(k, who):
        return wout.at[
            pl.ds(pl.multiple_of(who * Ch, 16), Ch), pl.ds(pl.multiple_of(k * OC, LANES), OC)
        ]

    def oz_copy(k, dz):
        src = w_output.at[pl.ds(pl.multiple_of(t * C + g * Ch, 16), Ch), :]
        return remote(
            src, o_piece(k, g), oz_s.at[dz], oz_r.at[dz], {"sp": lax.rem(s + dz, ns)}
        )

    def oy_copy(k, dz, dy, who):
        return remote(
            o_piece(k, who), o_piece(k, who), oy_s.at[dy - 1, dz], oy_r.at[dy - 1, dz],
            {"grp": lax.rem(g + dy, ng)},
        )

    def tok_copy(dt, slot):
        return remote(
            tokens, tok.at[slot], tok_s.at[dt], tok_r.at[dt], {"tp": lax.rem(t + dt, nt)}
        )

    def ext_copy(dt, slot):
        return remote(
            extra, ext.at[slot], ext_s.at[dt], ext_r.at[dt], {"tp": lax.rem(t + dt, nt)}
        )

    for a in range(3):
        own = weights[a].at[pl.ds(pl.multiple_of(g * Rh, 16), Rh), own_cols]

        @pl.when(s < ns - 1)
        def _():
            z_copy(s, a, 0, own).start()

        @pl.when(s > 0)
        def _():
            z_copy(s, a, 1, own).start()

    for dt in range(1, nt):
        tok_copy(dt, t).start()
        ext_copy(dt, t).start()
    locals_ = [
        pltpu.make_async_copy(tokens, tok.at[t], loc.at[0]),
        pltpu.make_async_copy(extra, ext.at[t], loc.at[1]),
        pltpu.make_async_copy(
            init.at[pl.ds(pl.multiple_of(t * C, LANES), C), :], start, loc.at[2]
        ),
        pltpu.make_async_copy(
            w_output.at[pl.ds(pl.multiple_of(t * C, LANES), C), :],
            wout.at[:, pl.ds(pl.multiple_of(s * OC, LANES), OC)],
            loc.at[3],
        ),
    ] + [
        pltpu.make_async_copy(
            weights[a].at[:, own_cols],
            wbuf.at[pl.ds(pl.multiple_of(s * R, 16), R), pl.ds(a * C, C)],
            loc.at[4 + a],
        )
        for a in range(3)
    ]
    for copy in locals_:
        copy.start()

    def normalize(slot):
        rows = 32

        def step(i, _):
            x = tok[slot, pl.ds(pl.multiple_of(i * rows, rows), rows), :].astype(F32)
            center = x - jnp.mean(x, axis=-1, keepdims=True)
            spread = jnp.mean(center * center, axis=-1, keepdims=True)
            nrm[pl.ds(pl.multiple_of(slot * span + i * rows, rows), rows), :] = (
                center * lax.rsqrt(spread + EPSILON) * norm_gain[...]
            ).astype(BF16)
            return 0

        lax.fori_loop(0, span // rows, step, 0)

    locals_[0].wait()
    normalize(t)

    for d in range(max(ns - 1, nt - 1)):
        if d < ns - 1:
            for a in range(3):
                for way in range(2):
                    k = s - 1 - d if way == 0 else s + 1 + d
                    valid = k >= 0 if way == 0 else k < ns
                    more = s < ns - 1 if way == 0 else s > 0

                    @pl.when(valid)
                    def _():
                        z_copy(k, a, way, piece(k, a, g)).wait_recv()

                        @pl.when(more)
                        def _():
                            z_copy(k, a, way, piece(k, a, g)).start()

                        for dy in range(1, ng):
                            y_copy(k, a, dy, g).start()
            if d == ns - 2:
                for dz in range(1, ns):
                    oz_copy(s, dz).start()
        if d < nt - 1:
            slot = lax.rem(t + nt - 1 - d, nt)
            tok_copy(d + 1, slot).wait_recv()
            normalize(slot)
            ext_copy(d + 1, slot).wait_recv()

    for copy in locals_[1:]:
        copy.wait()

    diag = same_group(C, C, HEAD)
    spread_eye = (lax.rem(iota((C, HEAD), 0), HEAD) == iota((C, HEAD), 1)).astype(F32)
    flipped = contract(spread_eye, start[...], 1, 1, HIGHEST)

    def y_wait(k, a):
        for dy in range(1, ng):
            y_copy(k, a, dy, lax.rem(g + ng - dy, ng)).wait_recv()

    for dz in range(1, ns):
        for a in range(3):
            y_wait(lax.rem(s + dz, ns), a)

    floor = gap[:, own_cols]
    heads = (
        iota((LANES, C), 0) == iota((LANES, C), 1) // HEAD + t * (C // HEAD)
    ).astype(F32)
    tri = (
        (iota((span, span), 0) >= iota((span, span), 1)) & same_group(span, span, BLOCK)
    ).astype(F32)
    carried[...] = jnp.zeros_like(carried)
    dk_send[...] = jnp.ones_like(dk_send)

    def project(m, _):
        rows = pl.ds(pl.multiple_of(m * span, span), span)
        x = nrm[rows, :]
        raw = [
            jnp.dot(x, wbuf[:, a * C:(a + 1) * C], preferred_element_type=F32).astype(BF16)
            for a in range(3)
        ]
        query = raw[0].astype(F32)
        query = query / (1.0 + jnp.exp(-query))
        key = floor / (1.0 + jnp.exp(raw[1].astype(F32)))
        log_keep = jnp.log1p(-key) + jnp.dot(
            ext[m], heads, precision=HIGHEST, preferred_element_type=F32
        )
        cumul = jnp.dot(tri, log_keep, precision=HIGHEST, preferred_element_type=F32)
        qd[rows, :] = (query * jnp.exp(cumul)).astype(BF16)
        kd[rows, :] = (key * jnp.exp(-cumul)).astype(BF16)
        val[rows, :] = raw[2]
        for b in range(per):
            part = slice(b * BLOCK, (b + 1) * BLOCK)
            total = cumul[(b + 1) * BLOCK - 1:(b + 1) * BLOCK, :]
            tail = (key[part] * jnp.exp(total - cumul[part])).astype(BF16)
            state = jnp.where(diag, contract(raw[2][part], tail, 0, 0), 0.0)
            decay = jnp.exp(total)
            n = m * per + b
            bstate[n] = state
            etot[n] = jnp.broadcast_to(decay, etot.shape[1:])
            carried[...] = carried[...] * decay + state
            dk_send[...] = dk_send[...] * decay
        return 0

    lax.fori_loop(0, nt, project, 0)

    tiles = [slice(i * LANES, (i + 1) * LANES) for i in range(G)]
    if fold:
        for i in range(G // 2):
            st_send[tiles[i], :] = (
                carried[tiles[2 * i], tiles[2 * i]]
                + swap_halves(carried[tiles[2 * i + 1], tiles[2 * i + 1]])
            ).astype(BF16)
    else:
        for i in range(G):
            st_send[tiles[i], :] = carried[tiles[i], tiles[i]].astype(BF16)

    def st_copy(dz, slot):
        return remote(st_send, st_recv.at[slot], st_s.at[dz], st_r.at[slot], {"sp": s + dz})

    def dk_copy(dz, slot):
        return remote(dk_send, dk_recv.at[slot], dk_s.at[dz], dk_r.at[slot], {"sp": s + dz})

    for dz in range(1, ns):
        @pl.when(s + dz < ns)
        def _():
            st_copy(dz, s).start()
            dk_copy(dz, s).start()

    for dz in range(1, ns):
        k = lax.rem(s + ns - dz, ns)
        oz_copy(k, dz).wait_recv()
        for dy in range(1, ng):
            oy_copy(k, dz, dy, g).start()

    copies = C // HEAD
    wide = copies * BLOCK
    causal = iota((BLOCK, wide), 0) >= lax.rem(iota((BLOCK, wide), 1), BLOCK)

    def inside(n, _):
        rows = pl.ds(pl.multiple_of(n * BLOCK, BLOCK), BLOCK)
        keys = jnp.where(diag, jnp.concatenate([kd[rows, :]] * copies, axis=0), 0.0)
        vals = jnp.where(diag, jnp.concatenate([val[rows, :]] * copies, axis=0), 0.0)
        scores = contract(qd[rows, :], keys.astype(BF16), 1, 1)
        scores = jnp.where(causal, scores, 0.0).astype(BF16)
        within[rows, :] = jnp.dot(scores, vals.astype(BF16), preferred_element_type=F32)
        return 0

    lax.fori_loop(0, nblk, inside, 0)

    carried[...] = jnp.where(diag, flipped, 0.0)
    near = same_group(LANES, LANES, HEAD)
    for k in range(ns - 1):
        @pl.when(k < s)
        def _():
            st_copy(1, k).wait_recv()
            dk_copy(1, k).wait_recv()
            decay = dk_recv[k][0:1, :]
            for i in range(G):
                packed = st_recv[k, tiles[i // 2] if fold else tiles[i], :].astype(F32)
                if fold and i % 2 == 1:
                    packed = swap_halves(packed)
                carried[tiles[i], tiles[i]] = carried[tiles[i], tiles[i]] * decay[
                    :, tiles[i]
                ] + jnp.where(near, packed, 0.0)

    ones = diag.astype(BF16)
    gain = head_gain[:, own_cols]

    def read(n, _):
        rows = pl.ds(pl.multiple_of(n * BLOCK, BLOCK), BLOCK)
        state = carried[...]
        out = within[rows, :] + contract(qd[rows, :], state.astype(BF16), 1, 1)
        power = jnp.dot((out * out).astype(BF16), ones, preferred_element_type=F32)
        gated[rows, :] = (
            out * lax.rsqrt(power * (1.0 / HEAD) + EPSILON) * gain
        ).astype(BF16)
        carried[...] = state * etot[n][0:1, :] + bstate[n]
        return 0

    lax.fori_loop(0, nblk, read, 0)

    rows_each = final.shape[0]
    here = s * nt + t

    def fin_copy(i, where):
        return remote(
            fin.at[pl.ds(i * rows_each, rows_each), :], fin_recv, fin_s.at[i], fin_r.at[0],
            {"sp": lax.div(where, nt), "tp": lax.rem(where, nt)},
        )

    own_piece = (s == ns - 1) & (here // ns == t)

    @pl.when(s == ns - 1)
    def _():
        fin[...] = contract(carried[...], spread_eye, 0, 0, HIGHEST)
        for i in range(ns):
            where = t * ns + i

            @pl.when(where != here)
            def _():
                fin_copy(i, where).start()

            @pl.when(where == here)
            def _():
                final[...] = fin[i * rows_each:(i + 1) * rows_each, :]

    for dz in range(1, ns):
        k = lax.rem(s + ns - dz, ns)
        for dy in range(1, ng):
            oy_copy(k, dz, dy, lax.rem(g + ng - dy, ng)).wait_recv()

    chip, core = lax.div(t, CORES), lax.rem(t, CORES)
    cw = O // chunks

    def product(dx, side, j):
        block = lax.rem(chip + dx, nx) * CORES + side
        x = gated[pl.ds(pl.multiple_of(block * span, span), span), :]
        return jnp.dot(x, wout[:, j * cw:(j + 1) * cw], preferred_element_type=F32)

    def a_copy(dx, j):
        return remote(
            a_send.at[dx, j], a_recv.at[dx, j], as_.at[dx, j], ar_.at[dx, j],
            {"tp": chip * CORES + 1 - core},
        )

    def b_copy(dx, j):
        return remote(
            b_send.at[dx, j], b_recv.at[dx, j], bs_.at[dx, j], br_.at[dx, j],
            {"tp": lax.rem(chip + dx, nx) * CORES + core},
        )

    order = list(range(1, nx)) + [0]
    for dx in order:
        for j in range(chunks):
            a_send[dx, j] = product(dx, 1 - core, j).astype(BF16)
            a_copy(dx, j).start()
        if dx:
            for j in range(chunks):
                mine = product(dx, core, j)
                a_copy(dx, j).wait_recv()
                b_send[dx, j] = (mine + a_recv[dx, j].astype(F32)).astype(BF16)
                b_copy(dx, j).start()
    for j in range(chunks):
        total = product(0, core, j)
        a_copy(0, j).wait_recv()
        total = total + a_recv[0, j].astype(F32)
        for dx in range(1, nx):
            b_copy(dx, j).wait_recv()
            total = total + b_recv[dx, j].astype(F32)
        mixed[:, j * cw:(j + 1) * cw] = total.astype(BF16)

    @pl.when(jnp.logical_not(own_piece))
    def _():
        fin_copy(0, here).wait_recv()
        final[...] = fin_recv[...]

    for a in range(3):
        for way in range(2):
            more = s < ns - 1 if way == 0 else s > 0
            for d in range(ns):
                k = s - d if way == 0 else s + d
                valid = k >= 0 if way == 0 else k < ns

                @pl.when(valid & more)
                def _():
                    z_copy(k, a, way, piece(k, a, g)).wait_send()
        for dz in range(1, ns):
            for dy in range(1, ng):
                y_copy(lax.rem(s + dz, ns), a, dy, g).wait_send()
    for dt in range(1, nt):
        tok_copy(dt, t).wait_send()
        ext_copy(dt, t).wait_send()
    for dz in range(1, ns):
        oz_copy(s, dz).wait_send()
        for dy in range(1, ng):
            oy_copy(lax.rem(s + ns - dz, ns), dz, dy, g).wait_send()

        @pl.when(s + dz < ns)
        def _():
            st_copy(dz, s).wait_send()
            dk_copy(dz, s).wait_send()

    @pl.when(s == ns - 1)
    def _():
        for i in range(ns):
            @pl.when(t * ns + i != here)
            def _():
                fin_copy(i, t * ns + i).wait_send()

    for dx in order:
        for j in range(chunks):
            a_copy(dx, j).wait_send()
            if dx:
                b_copy(dx, j).wait_send()


def body(
    tokens, norm_gain, w_query, w_forget, w_input, floor_gap, extra_decay, init_state,
    head_norm_gain, w_output,
):
    ng, ns, nt = lax.axis_size("grp"), lax.axis_size("sp"), lax.axis_size("tp")
    span, D = tokens.shape[1:]
    width, heads = w_query.shape[1], extra_decay.shape[2]
    C = width // nt
    O = w_output.shape[1] * ns
    chunks = 4
    T, nblk, nx = nt * span, nt * span // BLOCK, nt // CORES
    pack = C // 2 if (C // LANES) % 2 == 0 else C
    rows_each = width // (ns * nt)
    cw = O // chunks
    V, DMA = pltpu.VMEM, pltpu.SemaphoreType.DMA
    any_, vmem = pl.BlockSpec(memory_space=pl.ANY), pl.BlockSpec(memory_space=pltpu.VMEM)
    extra = jnp.pad(extra_decay[0], ((0, 0), (0, LANES - heads)))
    oth = max(ng - 1, 1)
    mixed, final = pl.pallas_call(
        functools.partial(kernel, (ng, ns, nt, span, D, C, O, chunks)),
        out_shape=(
            jax.ShapeDtypeStruct((span, O), BF16),
            jax.ShapeDtypeStruct((rows_each, HEAD), F32),
        ),
        in_specs=[any_, vmem, any_, any_, any_, vmem, any_, any_, vmem, any_],
        out_specs=(vmem, vmem),
        scratch_shapes=[
            V((nt, span, D), BF16), V((nt, span, LANES), F32), V((T, D), BF16),
            V((D, 3 * C), BF16), V((C, O), BF16), V((C, HEAD), F32),
            V((T, C), BF16), V((T, C), BF16), V((T, C), BF16),
            V((nblk, 8, C), F32), V((nblk, C, C), F32), V((T, C), F32), V((T, C), BF16),
            V((C, C), F32),
            V((pack, LANES), BF16), V((ns, pack, LANES), BF16), V((8, C), F32),
            V((ns, 8, C), F32), V((C, HEAD), F32), V((rows_each, HEAD), F32),
            V((nx, chunks, span, cw), BF16), V((nx, chunks, span, cw), BF16),
            V((nx, chunks, span, cw), BF16), V((nx, chunks, span, cw), BF16),
            DMA((7,)), DMA((nt,)), DMA((nt,)), DMA((nt,)), DMA((nt,)),
            DMA((2, ns, 3)), DMA((ns, 3)), DMA((oth, ns, 3)), DMA((oth, ns, 3)),
            DMA((ns,)), DMA((ns,)), DMA((oth, ns)), DMA((oth, ns)),
            DMA((ns,)), DMA((ns,)), DMA((ns,)), DMA((ns,)), DMA((ns,)), DMA((1,)),
            DMA((nx, chunks)), DMA((nx, chunks)), DMA((nx, chunks)), DMA((nx, chunks)),
        ],
        compiler_params=pltpu.CompilerParams(
            has_side_effects=True, vmem_limit_bytes=60 * 1024 * 1024
        ),
    )(
        tokens[0], norm_gain.astype(F32)[None], w_query, w_forget, w_input, floor_gap[None],
        extra, init_state.reshape(width, HEAD), head_norm_gain.astype(F32)[None], w_output,
    )
    return mixed[None], final.reshape(1, rows_each * HEAD)


def solution(mesh):
    placed = (
        P("grp", ("sp", "tp"), None),
        P(),
        P("sp", None),
        P("sp", None),
        P("sp", None),
        P(),
        P("grp", ("sp", "tp"), None),
        P("grp", None, None, None),
        P(),
        P(None, "sp"),
    )
    return jax.shard_map(
        body,
        mesh=mesh,
        in_specs=placed,
        out_specs=(P("grp", ("sp", "tp"), None), P("grp", ("sp", "tp"))),
        check_vma=False,
    )
```

```python
import functools

import jax
import jax.numpy as jnp
from jax import lax
from jax.experimental import pallas as pl
from jax.experimental.pallas import tpu as pltpu
from jax.sharding import PartitionSpec as P

HEAD = 64
BLOCK = 64
CORES = 2
LANES = 128
EPSILON = 1e-05
F32, BF16 = jnp.float32, jnp.bfloat16
HIGHEST = lax.Precision.HIGHEST


def contract(a, b, da, db, precision=None):
    return lax.dot_general(
        a, b, (((da,), (db,)), ((), ())), precision=precision, preferred_element_type=F32
    )


def iota(shape, dim):
    return lax.broadcasted_iota(jnp.int32, shape, dim)


def same_group(rows, cols, size):
    return iota((rows, cols), 0) // size == iota((rows, cols), 1) // size


def swap_halves(a):
    return jnp.concatenate([a[:, HEAD:], a[:, :HEAD]], axis=1)


def kernel(
    sizes,
    tokens, norm_gain, w_query, w_forget, w_input, gap, extra, init, head_gain, w_output,
    mixed, final,
    tok, ext, nrm, acc, wbuf, wout, start, qd, kd, val, etot, bstate, within, gated, carried,
    st_send, st_recv, dk_send, dk_recv, fin, fin_recv, a_send, a_recv, b_send, b_recv,
    loc, tok_s, tok_r, ext_s, ext_r, z_s, z_r, y_s, y_r, oz_s, oz_r, oy_s, oy_r,
    st_s, st_r, dk_s, dk_r, fin_s, fin_r, as_, ar_, bs_, br_,
):
    ng, ns, nt, span, D, C, O, chunks = sizes
    g, s, t = lax.axis_index("grp"), lax.axis_index("sp"), lax.axis_index("tp")
    R, OC = D // ns, O // ns
    Rh, Ch = R // ng, C // ng
    nx = nt // CORES
    T = nt * span
    nblk, per = T // BLOCK, span // BLOCK
    G = C // LANES
    fold = G % 2 == 0
    weights = (w_query, w_forget, w_input)
    here = s * nt + t
    chip, core = lax.div(t, CORES), lax.rem(t, CORES)
    partner = chip * CORES + 1 - core
    own_cols = pl.ds(pl.multiple_of(t * C, LANES), C)

    def remote(src, dst, ssem, rsem, where):
        return pltpu.make_async_remote_copy(
            src_ref=src, dst_ref=dst, send_sem=ssem, recv_sem=rsem,
            device_id=where, device_id_type=pl.DeviceIdType.MESH,
        )

    def piece(k, a, who):
        return wbuf.at[pl.ds(pl.multiple_of(k * R + who * Rh, 16), Rh), pl.ds(a * C, C)]

    def z_copy(k, a, way, src):
        to = s + 1 if way == 0 else s - 1
        return remote(src, piece(k, a, g), z_s.at[way, k, a], z_r.at[k, a], {"sp": to})

    def y_copy(k, a, dy, who):
        return remote(
            piece(k, a, who), piece(k, a, who), y_s.at[dy - 1, k, a], y_r.at[dy - 1, k, a],
            {"grp": lax.rem(g + dy, ng)},
        )

    def o_piece(k, who):
        return wout.at[
            pl.ds(pl.multiple_of(who * Ch, 16), Ch), pl.ds(pl.multiple_of(k * OC, LANES), OC)
        ]

    def oz_copy(k, way, src):
        to = s + 1 if way == 0 else s - 1
        return remote(src, o_piece(k, g), oz_s.at[way, k], oz_r.at[k], {"sp": to})

    def oy_copy(k, dy, who):
        return remote(
            o_piece(k, who), o_piece(k, who), oy_s.at[dy - 1, k], oy_r.at[dy - 1, k],
            {"grp": lax.rem(g + dy, ng)},
        )

    def from_chip(dx, side):
        return lax.rem(chip + nx - dx, nx) * CORES + side

    def tok_copy(src, slot, n, to):
        return remote(src, tok.at[slot], tok_s.at[n], tok_r.at[slot], {"tp": to})

    def tok_wait(slot):
        tok_copy(tokens, slot, 0, partner).wait_recv()

    def ext_copy(dt, slot):
        return remote(
            extra, ext.at[slot], ext_s.at[dt], ext_r.at[dt], {"tp": lax.rem(t + dt, nt)}
        )

    own_o = w_output.at[pl.ds(pl.multiple_of(t * C + g * Ch, 16), Ch), :]
    flows = [
        (way, (lambda d: s - 1 - d) if way == 0 else (lambda d: s + 1 + d),
         s if way == 0 else ns - 1 - s, (s < ns - 1) if way == 0 else (s > 0))
        for way in range(2)
    ]

    barrier = pltpu.get_barrier_semaphore()

    def greet(i, _):
        other = lax.rem(here + i, ns * nt)
        pl.semaphore_signal(
            barrier, inc=1, device_id={"sp": lax.div(other, nt), "tp": lax.rem(other, nt)},
            device_id_type=pl.DeviceIdType.MESH,
        )
        return 0

    for dy in range(1, ng):
        pl.semaphore_signal(
            barrier, inc=1, device_id={"grp": lax.rem(g + dy, ng)},
            device_id_type=pl.DeviceIdType.MESH,
        )
    lax.fori_loop(1, ns * nt, greet, 0)
    pl.semaphore_wait(barrier, ns * nt - 1 + ng - 1)

    for a in range(3):
        own = weights[a].at[pl.ds(pl.multiple_of(g * Rh, 16), Rh), own_cols]

        @pl.when(s < ns - 1)
        def _():
            z_copy(s, a, 0, own).start()

        @pl.when(s > 0)
        def _():
            z_copy(s, a, 1, own).start()

    for way, _, arrivals, more in flows:
        @pl.when((arrivals == 0) & more)
        def _():
            oz_copy(s, way, own_o).start()

    tok_copy(tokens, t, 0, partner).start()
    for dx in range(1, nx):
        to = lax.rem(chip + dx, nx) * CORES + core
        tok_copy(tokens, t, dx, to).start()
    for dt in range(1, nt):
        ext_copy(dt, t).start()
    locals_ = [
        pltpu.make_async_copy(tokens, tok.at[t], loc.at[0]),
        pltpu.make_async_copy(extra, ext.at[t], loc.at[1]),
        pltpu.make_async_copy(
            init.at[pl.ds(pl.multiple_of(t * C, LANES), C), :], start, loc.at[2]
        ),
        pltpu.make_async_copy(
            w_output.at[pl.ds(pl.multiple_of(t * C, LANES), C), :],
            wout.at[:, pl.ds(pl.multiple_of(s * OC, LANES), OC)],
            loc.at[3],
        ),
    ] + [
        pltpu.make_async_copy(
            weights[a].at[:, own_cols],
            wbuf.at[pl.ds(pl.multiple_of(s * R, 16), R), pl.ds(a * C, C)],
            loc.at[4 + a],
        )
        for a in range(3)
    ]
    for copy in locals_:
        copy.start()

    def normalize(slot):
        rows = 32

        def step(i, _):
            x = tok[slot, pl.ds(pl.multiple_of(i * rows, rows), rows), :].astype(F32)
            center = x - jnp.mean(x, axis=-1, keepdims=True)
            spread = jnp.mean(center * center, axis=-1, keepdims=True)
            nrm[pl.ds(pl.multiple_of(slot * span + i * rows, rows), rows), :] = (
                center * lax.rsqrt(spread + EPSILON) * norm_gain[...]
            ).astype(BF16)
            return 0

        lax.fori_loop(0, span // rows, step, 0, unroll=True)

    locals_[0].wait()
    normalize(t)

    tok_wait(partner)
    normalize(partner)

    for d in range(ns - 1):
        for a in range(3):
            for way, shard, arrivals, more in flows:
                k = shard(d)

                @pl.when(d < arrivals)
                def _():
                    z_copy(k, a, way, piece(k, a, g)).wait_recv()

                    @pl.when(more)
                    def _():
                        z_copy(k, a, way, piece(k, a, g)).start()

                    for dy in range(1, ng):
                        y_copy(k, a, dy, g).start()
        for way, _, arrivals, more in flows:
            @pl.when((arrivals == d + 1) & more)
            def _():
                oz_copy(s, way, own_o).start()
        if d == min(1, ns - 2):
            for dx in range(1, nx):
                slot = from_chip(dx, core)
                tok_wait(slot)
                tok_copy(tok.at[slot], slot, nx - 1 + dx, partner).start()
                normalize(slot)
    for dx in range(1, nx):
        slot = from_chip(dx, 1 - core)
        tok_wait(slot)
        normalize(slot)

    def o_step(e, onward):
        for way, shard, arrivals, more in flows:
            k = shard(e)
            when = (e < arrivals) & (more if onward else jnp.logical_not(more))

            @pl.when(when)
            def _():
                oz_copy(k, way, own_o).wait_recv()
                if onward:
                    oz_copy(k, way, o_piece(k, g)).start()
                for dy in range(1, ng):
                    oy_copy(k, dy, g).start()

    for e in range(ns - 1):
        o_step(e, True)

    for copy in locals_[1:]:
        copy.wait()

    diag = same_group(C, C, HEAD)
    spread_eye = (lax.rem(iota((C, HEAD), 0), HEAD) == iota((C, HEAD), 1)).astype(F32)
    flipped = contract(spread_eye, start[...], 1, 1, HIGHEST)

    def y_wait(k, a):
        for dy in range(1, ng):
            y_copy(k, a, dy, lax.rem(g + ng - dy, ng)).wait_recv()

    def add(k, first):
        deep = pl.ds(pl.multiple_of(k * R, LANES), R)

        def step(m, _):
            rows = pl.ds(pl.multiple_of(m * span, span), span)
            more = jnp.dot(nrm[rows, deep], wbuf[deep, :], preferred_element_type=F32)
            acc[rows, :] = more if first else acc[rows, :] + more
            return 0

        lax.fori_loop(0, nt, step, 0)

    add(s, True)
    for d in range(ns - 1):
        for _, shard, arrivals, _ in flows:
            k = shard(d)

            @pl.when(d < arrivals)
            def _():
                for a in range(3):
                    y_wait(k, a)
                add(k, False)

    for dt in range(1, nt):
        ext_copy(dt, lax.rem(t + nt - dt, nt)).wait_recv()

    floor = gap[:, own_cols]
    heads = (
        iota((ext.shape[1], C), 0) == iota((ext.shape[1], C), 1) // HEAD + t * (C // HEAD)
    ).astype(F32)
    tri = (
        (iota((span, span), 0) >= iota((span, span), 1)) & same_group(span, span, BLOCK)
    ).astype(F32)
    carried[...] = jnp.zeros_like(carried)
    dk_send[...] = jnp.ones_like(dk_send)

    def project(m, _):
        rows = pl.ds(pl.multiple_of(m * span, span), span)
        raw = [acc[rows, a * C:(a + 1) * C].astype(BF16) for a in range(3)]
        query = raw[0].astype(F32)
        query = query / (1.0 + jnp.exp(-query))
        key = floor / (1.0 + jnp.exp(raw[1].astype(F32)))
        log_keep = jnp.log1p(-key) + contract(ext[m], heads, 0, 0, HIGHEST)
        cumul = jnp.dot(tri, log_keep, precision=HIGHEST, preferred_element_type=F32)
        qd[rows, :] = (query * jnp.exp(cumul)).astype(BF16)
        kd[rows, :] = (key * jnp.exp(-cumul)).astype(BF16)
        val[rows, :] = raw[2]
        for b in range(per):
            part = slice(b * BLOCK, (b + 1) * BLOCK)
            total = cumul[(b + 1) * BLOCK - 1:(b + 1) * BLOCK, :]
            tail = (key[part] * jnp.exp(total - cumul[part])).astype(BF16)
            state = jnp.where(diag, contract(raw[2][part], tail, 0, 0), 0.0)
            decay = jnp.exp(total)
            n = m * per + b
            bstate[n] = state
            etot[n] = jnp.broadcast_to(decay, etot.shape[1:])
            carried[...] = carried[...] * decay + state
            dk_send[...] = dk_send[...] * decay
        return 0

    half = nt // 2
    lax.fori_loop(0, half, project, 0)
    o_step(0, False)
    lax.fori_loop(half, nt, project, 0)

    tiles = [slice(i * LANES, (i + 1) * LANES) for i in range(G)]
    if fold:
        for i in range(G // 2):
            st_send[tiles[i], :] = (
                carried[tiles[2 * i], tiles[2 * i]]
                + swap_halves(carried[tiles[2 * i + 1], tiles[2 * i + 1]])
            ).astype(BF16)
    else:
        for i in range(G):
            st_send[tiles[i], :] = carried[tiles[i], tiles[i]].astype(BF16)

    def st_copy(dz, slot):
        return remote(st_send, st_recv.at[slot], st_s.at[dz], st_r.at[slot], {"sp": s + dz})

    def dk_copy(dz, slot):
        return remote(dk_send, dk_recv.at[slot], dk_s.at[dz], dk_r.at[slot], {"sp": s + dz})

    for dz in range(1, ns):
        @pl.when(s + dz < ns)
        def _():
            st_copy(dz, s).start()
            dk_copy(dz, s).start()

    for e in range(1, ns - 1):
        o_step(e, False)

    copies = C // HEAD
    wide = copies * BLOCK
    causal = iota((BLOCK, wide), 0) >= lax.rem(iota((BLOCK, wide), 1), BLOCK)

    def inside(n, _):
        rows = pl.ds(pl.multiple_of(n * BLOCK, BLOCK), BLOCK)
        keys = jnp.where(diag, jnp.concatenate([kd[rows, :]] * copies, axis=0), 0.0)
        vals = jnp.where(diag, jnp.concatenate([val[rows, :]] * copies, axis=0), 0.0)
        scores = contract(qd[rows, :], keys.astype(BF16), 1, 1)
        scores = jnp.where(causal, scores, 0.0).astype(BF16)
        within[rows, :] = jnp.dot(scores, vals.astype(BF16), preferred_element_type=F32)
        return 0

    lax.fori_loop(0, nblk, inside, 0)

    carried[...] = jnp.where(diag, flipped, 0.0)
    near = same_group(LANES, LANES, HEAD)
    for k in range(ns - 1):
        @pl.when(k < s)
        def _():
            st_copy(1, k).wait_recv()
            dk_copy(1, k).wait_recv()
            decay = dk_recv[k][0:1, :]
            for i in range(G):
                packed = st_recv[k, tiles[i // 2] if fold else tiles[i], :].astype(F32)
                if fold and i % 2 == 1:
                    packed = swap_halves(packed)
                carried[tiles[i], tiles[i]] = carried[tiles[i], tiles[i]] * decay[
                    :, tiles[i]
                ] + jnp.where(near, packed, 0.0)

    ones = diag.astype(BF16)
    gain = head_gain[:, own_cols]

    def read(n, _):
        rows = pl.ds(pl.multiple_of(n * BLOCK, BLOCK), BLOCK)
        state = carried[...]
        out = within[rows, :] + contract(qd[rows, :], state.astype(BF16), 1, 1)
        power = jnp.dot((out * out).astype(BF16), ones, preferred_element_type=F32)
        gated[rows, :] = (
            out * lax.rsqrt(power * (1.0 / HEAD) + EPSILON) * gain
        ).astype(BF16)
        carried[...] = state * etot[n][0:1, :] + bstate[n]
        return 0

    lax.fori_loop(0, nblk, read, 0)

    rows_each = final.shape[0]
    def fin_copy(i, where):
        return remote(
            fin.at[pl.ds(i * rows_each, rows_each), :], fin_recv, fin_s.at[i], fin_r.at[0],
            {"sp": lax.div(where, nt), "tp": lax.rem(where, nt)},
        )

    own_piece = (s == ns - 1) & (here // ns == t)

    @pl.when(s == ns - 1)
    def _():
        fin[...] = contract(carried[...], spread_eye, 0, 0, HIGHEST)
        for i in range(ns):
            where = t * ns + i

            @pl.when(where != here)
            def _():
                fin_copy(i, where).start()

            @pl.when(where == here)
            def _():
                final[...] = fin[i * rows_each:(i + 1) * rows_each, :]

    for dz in range(1, ns):
        for dy in range(1, ng):
            oy_copy(lax.rem(s + dz, ns), dy, lax.rem(g + ng - dy, ng)).wait_recv()

    cw = O // chunks

    def product(dx, side, j):
        block = lax.rem(chip + dx, nx) * CORES + side
        x = gated[pl.ds(pl.multiple_of(block * span, span), span), :]
        return jnp.dot(x, wout[:, j * cw:(j + 1) * cw], preferred_element_type=F32)

    def a_copy(dx, j):
        return remote(
            a_send.at[dx, j], a_recv.at[dx, j], as_.at[dx, j], ar_.at[dx, j],
            {"tp": partner},
        )

    def b_copy(dx, j):
        return remote(
            b_send.at[dx, j], b_recv.at[dx, j], bs_.at[dx, j], br_.at[dx, j],
            {"tp": lax.rem(chip + dx, nx) * CORES + core},
        )

    order = list(range(1, nx)) + [0]
    for dx in order:
        for j in range(chunks):
            a_send[dx, j] = product(dx, 1 - core, j).astype(BF16)
            a_copy(dx, j).start()
        if dx:
            for j in range(chunks):
                mine = product(dx, core, j)
                a_copy(dx, j).wait_recv()
                b_send[dx, j] = (mine + a_recv[dx, j].astype(F32)).astype(BF16)
                b_copy(dx, j).start()
    for j in range(chunks):
        total = product(0, core, j)
        a_copy(0, j).wait_recv()
        total = total + a_recv[0, j].astype(F32)
        for dx in range(1, nx):
            b_copy(dx, j).wait_recv()
            total = total + b_recv[dx, j].astype(F32)
        mixed[:, j * cw:(j + 1) * cw] = total.astype(BF16)

    @pl.when(jnp.logical_not(own_piece))
    def _():
        fin_copy(0, here).wait_recv()
        final[...] = fin_recv[...]

    for a in range(3):
        for way in range(2):
            more = s < ns - 1 if way == 0 else s > 0
            for d in range(ns):
                k = s - d if way == 0 else s + d
                valid = k >= 0 if way == 0 else k < ns

                @pl.when(valid & more)
                def _():
                    z_copy(k, a, way, piece(k, a, g)).wait_send()
        for dz in range(1, ns):
            for dy in range(1, ng):
                y_copy(lax.rem(s + dz, ns), a, dy, g).wait_send()
    for way, _, arrivals, more in flows:
        for d in range(ns):
            k = s - d if way == 0 else s + d

            @pl.when((d <= arrivals) & more)
            def _():
                oz_copy(k, way, own_o).wait_send()
    for n in range(2 * nx - 1):
        tok_copy(tokens, t, n, partner).wait_send()
    for dt in range(1, nt):
        ext_copy(dt, t).wait_send()
    for dz in range(1, ns):
        for dy in range(1, ng):
            oy_copy(lax.rem(s + dz, ns), dy, g).wait_send()

        @pl.when(s + dz < ns)
        def _():
            st_copy(dz, s).wait_send()
            dk_copy(dz, s).wait_send()

    @pl.when(s == ns - 1)
    def _():
        for i in range(ns):
            @pl.when(t * ns + i != here)
            def _():
                fin_copy(i, t * ns + i).wait_send()

    for dx in order:
        for j in range(chunks):
            a_copy(dx, j).wait_send()
            if dx:
                b_copy(dx, j).wait_send()


def body(
    tokens, norm_gain, w_query, w_forget, w_input, floor_gap, extra_decay, init_state,
    head_norm_gain, w_output,
):
    ng, ns, nt = lax.axis_size("grp"), lax.axis_size("sp"), lax.axis_size("tp")
    span, D = tokens.shape[1:]
    width, heads = w_query.shape[1], extra_decay.shape[2]
    C = width // nt
    O = w_output.shape[1] * ns
    chunks = 4
    T, nblk, nx = nt * span, nt * span // BLOCK, nt // CORES
    pack = C // 2 if (C // LANES) % 2 == 0 else C
    rows_each = width // (ns * nt)
    cw = O // chunks
    V, DMA = pltpu.VMEM, pltpu.SemaphoreType.DMA
    any_, vmem = pl.BlockSpec(memory_space=pl.ANY), pl.BlockSpec(memory_space=pltpu.VMEM)
    extra = extra_decay[0].T
    oth = max(ng - 1, 1)
    mixed, final = pl.pallas_call(
        functools.partial(kernel, (ng, ns, nt, span, D, C, O, chunks)),
        out_shape=(
            jax.ShapeDtypeStruct((span, O), BF16),
            jax.ShapeDtypeStruct((rows_each, HEAD), F32),
        ),
        in_specs=[any_, vmem, any_, any_, any_, vmem, any_, any_, vmem, any_],
        out_specs=(vmem, vmem),
        scratch_shapes=[
            V((nt, span, D), BF16), V((nt, heads, span), F32), V((T, D), BF16), V((T, 3 * C), F32),
            V((D, 3 * C), BF16), V((C, O), BF16), V((C, HEAD), F32),
            V((T, C), BF16), V((T, C), BF16), V((T, C), BF16),
            V((nblk, 8, C), F32), V((nblk, C, C), F32), V((T, C), F32), V((T, C), BF16),
            V((C, C), F32),
            V((pack, LANES), BF16), V((ns, pack, LANES), BF16), V((8, C), F32),
            V((ns, 8, C), F32), V((C, HEAD), F32), V((rows_each, HEAD), F32),
            V((nx, chunks, span, cw), BF16), V((nx, chunks, span, cw), BF16),
            V((nx, chunks, span, cw), BF16), V((nx, chunks, span, cw), BF16),
            DMA((7,)), DMA((2 * nx,)), DMA((nt,)), DMA((nt,)), DMA((nt,)),
            DMA((2, ns, 3)), DMA((ns, 3)), DMA((oth, ns, 3)), DMA((oth, ns, 3)),
            DMA((2, ns)), DMA((ns,)), DMA((oth, ns)), DMA((oth, ns)),
            DMA((ns,)), DMA((ns,)), DMA((ns,)), DMA((ns,)), DMA((ns,)), DMA((1,)),
            DMA((nx, chunks)), DMA((nx, chunks)), DMA((nx, chunks)), DMA((nx, chunks)),
        ],
        compiler_params=pltpu.CompilerParams(
            collective_id=0, has_side_effects=True, vmem_limit_bytes=60 * 1024 * 1024
        ),
    )(
        tokens[0], norm_gain.astype(F32)[None], w_query, w_forget, w_input, floor_gap[None],
        extra, init_state.reshape(width, HEAD), head_norm_gain.astype(F32)[None], w_output,
    )
    return mixed[None], final.reshape(1, rows_each * HEAD)


def solution(mesh):
    placed = (
        P("grp", ("sp", "tp"), None),
        P(),
        P("sp", None),
        P("sp", None),
        P("sp", None),
        P(),
        P("grp", ("sp", "tp"), None),
        P("grp", None, None, None),
        P(),
        P(None, "sp"),
    )
    return jax.shard_map(
        body,
        mesh=mesh,
        in_specs=placed,
        out_specs=(P("grp", ("sp", "tp"), None), P("grp", ("sp", "tp"))),
        check_vma=False,
    )
```
